32 devices in a mesh: ep: 4 (over y, x), tp: 8 (over z, core).
Axes of the slice: x: 2, y: 2, z: 4, core: 2. Of those that a mesh axis runs over, the one named last changes fastest.
Arguments:
- tokens: bfloat16 [1024, 2048], P('ep', 'tp'), may hold values from -600 to 600
- pre_gain: float32 [2048], P('tp'), may hold values from 0.1 to 1.9
- expert_gate: bfloat16 [4, 2048, 8192], P('ep', None, 'tp'), may hold values from -0.125 to 0.125
- expert_up: bfloat16 [4, 2048, 8192], P('ep', None, 'tp'), may hold values from -0.125 to 0.125
- expert_down: bfloat16 [4, 8192, 2048], P('ep', 'tp'), may hold values from -8 to 8
- routes: int32 [1024, 2], P('ep'), may hold values from 0 to 3, all different within a row; in each aligned block of 256 rows (0 to 255, 256 to 511, ...) at most 192 rows name the same one
- route_weights: float32 [1024, 2], P('ep'), may hold values from 0.1 to 1
- post_gain: float32 [2048], P('tp'), may hold values from 0.1 to 1.9
Outputs:
- layer_out: bfloat16 [1024, 2048], P('ep', 'tp')
The draws below stay inside these ranges and needn't reach their ends.
Inputs may be any that keep to these rules, and one draw needn't show every extreme that they name: `routes`: each token names 2 different experts. Among the 256 tokens of one index of ep no expert is named more than 192 times, a bound that some expert reaches in some of these blocks.
All inputs are finite; a program needn't handle non-finite values.
Results may differ from the reference program's by a relative error of at most 0.024.
Values may be sent and summed in bfloat16 or wider, within the bound.
A program may use at most 64 MiB of HBM per device.

```python
import math
import jax
import jax.numpy as jnp
import numpy as np
from jax import lax

D = 2048
FF = 8192
TOPK = 2
TOK_EP = 256
EXPERTS = 4
CAP = 192
TOKENS = 1024
N_EP = 4
N_TP = 8


def column_scale(key, count):
    ramp = jnp.arange(count, dtype=jnp.float32) / max(count - 1, 1)
    rough = jax.random.uniform(key, (count,), jnp.float32, -0.35, 0.35)
    return jnp.exp(math.log(10.0) * ramp + rough)


def draw_tokens(key, part):
    keys = jax.random.split(jax.random.fold_in(key, 11), 3)
    entries = jnp.clip(jax.random.normal(keys[0], (TOKENS, D), jnp.float32), -4.0, 4.0)
    row_scale = jnp.exp(jax.random.uniform(keys[1], (TOKENS, 1), jnp.float32, 0.0, math.log(10.0)))
    return (entries * row_scale * column_scale(keys[2], D)[None, :]).astype(jnp.bfloat16)


def draw_expert_down(key, part):
    keys = jax.random.split(jax.random.fold_in(key, 23), 2)
    entries = jnp.clip(jax.random.normal(keys[0], (EXPERTS, FF, D), jnp.float32), -4.0, 4.0)
    scaled = entries * FF ** (-0.5) * column_scale(keys[1], D)[None, None, :]
    return scaled.astype(jnp.bfloat16)


def shard_levels(stream_key, extent, cuts, least, top_value):
    level = 1.0
    for axis_at, shards_of in cuts:
        heights = jax.random.uniform(jax.random.fold_in(jax.random.fold_in(stream_key, 6), axis_at), (shards_of,), jnp.float32, least / len(cuts), top_value / len(cuts))
        level = level * jnp.repeat(jnp.exp(heights), extent[axis_at] // shards_of).reshape((-1,) + (1,) * (len(extent) - 1 - axis_at))
    return level


def shared_out(key, own, number, rows, amount, top, limit, skew):
    ranking = jax.random.permutation(key, amount)
    crowded, usual = shares(amount, rows * top, limit, skew, True), shares(amount, rows * top, limit, skew, False)
    places = jnp.arange(amount)

    def named(lengths, offset_by):
        used = int((lengths > 0).sum())
        fixed = max(1, used // 4)
        shifted = fixed + (places - fixed + offset_by * (used - fixed)) % max(1, amount - fixed)
        return jnp.zeros((amount,), jnp.int32).at[ranking[jnp.where(places < fixed, places, shifted)]].set(jnp.asarray(lengths, jnp.int32))

    lengths = jnp.where(number % 4 == 0, named(crowded, number // 4), named(usual, number - number // 4 - 1))
    mixed = jax.random.permutation(jax.random.fold_in(own, 3), amount)
    source_of, receiver = mixed[0:amount // 2 * 2:2], mixed[1:amount // 2 * 2:2]
    margin = jnp.minimum(lengths[source_of] - 1, limit - lengths[receiver]) // 2
    margin = jnp.where((source_of == ranking[0]) | (receiver == ranking[0]) | (lengths[receiver] == 0), 0, jnp.maximum(margin, 0))
    shifted = jax.random.randint(jax.random.fold_in(own, 4), (amount // 2,), 0, 1 << 20) % (margin + 1)
    lengths = lengths.at[source_of].add(-shifted).at[receiver].add(shifted)
    items = jnp.searchsorted(jnp.cumsum(lengths), jnp.arange(rows * top), side="right").astype(jnp.int32)
    table = items.reshape(top, rows).T
    table = table[jax.random.permutation(jax.random.fold_in(own, 1), rows)]
    offset_by = jax.random.randint(jax.random.fold_in(own, 2), (rows, 1), 0, top)
    return jnp.take_along_axis(table, (jnp.arange(top)[None, :] + offset_by) % top, axis=1)


def shares(amount, total, reach, slope, full):
    weights = [(1 << 20) // math.isqrt(grade ** slope) + 1 for grade in range(1, amount + 1)]
    largest = reach if full else min(reach, max(-(-total // amount), total * weights[0] // sum(weights)))
    least = 1 if total - largest >= amount - 1 else 0
    counts, rest = [largest] + [least] * (amount - 1), total - largest - least * (amount - 1)
    while rest > 0:
        candidates = [i for i in range(1, amount) if counts[i] < largest] or [i for i in range(1, amount) if counts[i] < reach]
        mass, left = sum([weights[i] for i in candidates]), rest
        for i in candidates:
            extra = min(reach - counts[i], max(1, left * weights[i] // mass), rest)
            counts[i] = counts[i] + extra
            rest = rest - extra
    return np.array(counts)


def gaussian(stream_key, dims, spread, most, cuts=(), held_as=jnp.bfloat16):
    values = spread * jax.random.normal(stream_key, dims, jnp.float32)
    if cuts:
        values = values * shard_levels(stream_key, dims, cuts, -0.22, 0.18)
    return jnp.clip(values, -most, most).astype(held_as)


def setup_inputs(seed: int = 0) -> dict:
    key_of = jax.random.split(jax.random.key(seed), 9)
    tokens = draw_tokens(jax.random.fold_in(key_of[8], 71), 0)
    pre_gain = jnp.clip(1.0 + 0.18 * jax.random.normal(key_of[1], (D,), jnp.float32), 0.1, 1.9)
    expert_gate = gaussian(key_of[2], (EXPERTS, D, FF), D ** -0.5, 0.125, ((0, 4), (2, 8)))
    expert_up = gaussian(key_of[3], (EXPERTS, D, FF), D ** -0.5, 0.125, ((0, 4), (2, 8)))
    expert_down = draw_expert_down(jax.random.fold_in(key_of[8], 71), 0)
    routes_keys = jax.random.split(jax.random.fold_in(key_of[5], 1), TOKENS // TOK_EP)
    routes_turns = jax.random.permutation(jax.random.fold_in(key_of[5], 3), TOKENS // TOK_EP)
    routes = jax.vmap(lambda own, number: shared_out(jax.random.fold_in(key_of[5], 2), own, number, TOK_EP, EXPERTS, TOPK, CAP, 2))(routes_keys, routes_turns).reshape((TOKENS, TOPK))
    route_weights = jnp.clip(0.1 + 0.9 * jax.random.uniform(key_of[6], (TOKENS, TOPK), jnp.float32) ** shard_levels(key_of[6], (TOKENS, TOPK), ((0, 4),), -0.2, 0.2), 0.1, 1.0)
    post_gain = jnp.clip(1.0 + 0.18 * jax.random.normal(key_of[7], (D,), jnp.float32), 0.1, 1.9)
    return {"tokens": tokens, "pre_gain": pre_gain, "expert_gate": expert_gate, "expert_up": expert_up, "expert_down": expert_down, "routes": routes, "route_weights": route_weights, "post_gain": post_gain}


EPSILON = 1e-06

def rms_scale(values, gain):
    return values * lax.rsqrt(lax.optimization_barrier(jnp.mean(values * values, axis=-1, keepdims=True)) + EPSILON) * gain.astype(jnp.float32)

def reference(tokens, pre_gain, expert_gate, expert_up, expert_down, routes, route_weights, post_gain):
    normed = rms_scale(tokens.astype(jnp.float32), pre_gain).astype(jnp.bfloat16)
    blocks = routes.reshape(N_EP, TOK_EP, TOPK).astype(jnp.int32)
    onehot = (blocks[..., None] == jnp.arange(EXPERTS, dtype=jnp.int32)).astype(jnp.int32)
    onehot = onehot.reshape(N_EP, TOK_EP * TOPK, EXPERTS)
    earlier = jnp.cumsum(onehot, axis=1) - onehot
    slots = lax.optimization_barrier(jnp.sum(earlier * onehot, axis=-1)).reshape(N_EP, TOK_EP, TOPK).astype(jnp.int32)
    block_ids = jnp.broadcast_to(jnp.arange(N_EP, dtype=jnp.int32)[:, None, None], blocks.shape)
    token_ids = jnp.broadcast_to(block_ids * TOK_EP + jnp.arange(TOK_EP, dtype=jnp.int32)[None, :, None], blocks.shape)
    table = jnp.full((EXPERTS, N_EP, CAP), TOKENS, jnp.int32).at[blocks, block_ids, slots].set(token_ids)
    padded = jnp.concatenate([normed, jnp.zeros((1, D), jnp.bfloat16)], axis=0)
    row_count = N_EP * CAP
    part_units = FF // N_TP

    def one_expert(args):
        row_index, w_gate, w_up, w_down = args
        rows = padded[row_index.reshape(-1)]
        gate_pre = jnp.dot(rows, w_gate, preferred_element_type=jnp.float32)
        up_pre = jnp.dot(rows, w_up, preferred_element_type=jnp.float32)
        hidden = (jax.nn.silu(gate_pre) * up_pre).astype(jnp.bfloat16)
        hidden_blocks = hidden.reshape(row_count, N_TP, part_units).transpose(1, 0, 2)
        weight_blocks = w_down.reshape(N_TP, part_units, D)

        def add_block(running, pair):
            part_hidden, part_weight = pair
            partial_value = jnp.dot(part_hidden, part_weight, preferred_element_type=jnp.float32)
            rounded = lax.optimization_barrier(partial_value.astype(jnp.bfloat16))
            return (running + rounded.astype(jnp.float32), None)
        running, _ = lax.scan(add_block, jnp.zeros((row_count, D), jnp.float32), (hidden_blocks, weight_blocks))
        return running.astype(jnp.bfloat16)
    outputs = lax.map(one_expert, (table, expert_gate, expert_up, expert_down))
    picked = outputs[blocks, block_ids * CAP + slots].reshape(TOKENS, TOPK, D)
    combined = lax.optimization_barrier(jnp.sum(route_weights[:, :, None] * picked.astype(jnp.float32), axis=1))
    return rms_scale(combined, post_gain).astype(jnp.bfloat16)
```

```python
import functools

import jax
import jax.numpy as jnp
from jax import lax
from jax.experimental import pallas as pl
from jax.experimental.pallas import tpu as pltpu
from jax.sharding import PartitionSpec as P

EPSILON = 1e-06


def local(tokens, pre_gain, expert_gate, expert_up, expert_down, routes, route_weights, post_gain):
    local_experts = expert_gate.shape[0]
    groups = lax.axis_size("ep")
    experts_all = local_experts * groups
    tok_rows, part_width = tokens.shape
    full_width = part_width * lax.axis_size("tp")
    capacity = 3 * tok_rows // experts_all
    values = tokens.astype(jnp.float32)
    input_sq = lax.psum(jnp.sum(values * values, axis=-1), "tp")
    normed = (
        values * lax.rsqrt(input_sq / full_width + EPSILON)[:, None] * pre_gain[None, :]
    ).astype(jnp.bfloat16)
    onehot = (routes[:, :, None] == jnp.arange(experts_all, dtype=jnp.int32)).astype(jnp.int32)
    onehot = onehot.reshape(tok_rows * 2, experts_all)
    earlier = jnp.cumsum(onehot, axis=0) - onehot
    slots = jnp.sum(earlier * onehot, axis=-1).reshape(tok_rows, 2)
    positions = routes * capacity + slots
    places = jnp.arange(experts_all * capacity, dtype=jnp.int32)
    first_pick = (places[:, None] == positions[None, :, 0]).astype(jnp.bfloat16)
    second_pick = (places[:, None] == positions[None, :, 1]).astype(jnp.bfloat16)
    dispatch = first_pick + second_pick
    outgoing = jnp.dot(dispatch, normed, preferred_element_type=jnp.float32).astype(jnp.bfloat16)
    arrived = lax.all_to_all(outgoing, "ep", split_axis=0, concat_axis=0, tiled=True)
    fragment = lax.all_gather(arrived, "tp", axis=1, tiled=True)
    count = fragment.shape[1]
    grouped = fragment.reshape(groups, local_experts, capacity, count)
    gate_pre = jnp.einsum(
        "secw,ewf->secf", grouped, expert_gate, preferred_element_type=jnp.float32
    )
    up_pre = jnp.einsum("secw,ewf->secf", grouped, expert_up, preferred_element_type=jnp.float32)
    hidden = (jax.nn.silu(gate_pre) * up_pre).astype(jnp.bfloat16)
    product = jnp.einsum("secf,efd->dsec", hidden, expert_down, preferred_element_type=jnp.float32)
    summed = lax.psum_scatter(
        product.reshape(lax.axis_size("tp") * part_width, groups * local_experts * capacity).astype(
            jnp.bfloat16
        ),
        "tp",
        scatter_dimension=0,
        tiled=True,
    )
    returned = lax.all_to_all(summed, "ep", split_axis=1, concat_axis=1, tiled=True)
    contract = (((0,), (1,)), ((), ()))
    first_out = lax.dot_general(first_pick, returned, contract, preferred_element_type=jnp.float32)
    second_out = lax.dot_general(
        second_pick, returned, contract, preferred_element_type=jnp.float32
    )
    combined = route_weights[:, 0:1] * first_out + route_weights[:, 1:2] * second_out
    output_sq = lax.psum(jnp.sum(combined * combined, axis=-1), "tp")
    scaled = combined * lax.rsqrt(output_sq / full_width + EPSILON)[:, None] * post_gain[None, :]
    return scaled.astype(jnp.bfloat16)


CORES = 2
F32 = jnp.float32
BF16 = jnp.bfloat16
EXACT = lax.Precision.HIGHEST
MESH = pl.DeviceIdType.MESH


def flip(index, bits):
    place = 1
    while place <= bits:
        if bits & place:
            index = index + place - 2 * place * lax.rem(lax.div(index, place), 2)
        place *= 2
    return index


def flip_traced(index, bits, size):
    total, place = 0, 1
    while place < size:
        total = total + place * lax.rem(lax.div(index, place) + lax.div(bits, place), 2)
        place *= 2
    return total


def fused(
    groups, parts, tok, gain, route, weight, gate_hbm, up_hbm, down_hbm, post, out,
    zbuf, gains, disp, mix, hi, lo, xsend, x, squares, gate, up, down, acc_gate, acc_up,
    hidden, half, own, half_in, back, ret, zsend, zin, stats,
    wsem, zs, zr, gs, gr, xs, xr, fs, fr, ds, dr, qs, qr, cs, cr, ps, pr,
):
    t, e = lax.axis_index("tp"), lax.axis_index("ep")
    z, c = lax.div(t, CORES), lax.rem(t, CORES)
    levels = parts // CORES
    rows, width = tok.shape
    cap = disp.shape[1]
    full = parts * width

    barrier = pltpu.get_barrier_semaphore()
    for i in range(1, parts):
        pl.semaphore_signal(barrier, inc=1, device_id={"tp": flip(t, i)}, device_id_type=MESH)
    for d in range(1, groups):
        pl.semaphore_signal(barrier, inc=1, device_id={"ep": flip(e, d)}, device_id_type=MESH)

    loads = [
        pltpu.make_async_copy(gate_hbm.at[0], gate, wsem.at[0]),
        pltpu.make_async_copy(up_hbm.at[0], up, wsem.at[1]),
        pltpu.make_async_copy(down_hbm.at[0], down, wsem.at[2]),
    ]
    for load in loads:
        load.start()

    def remote(src, dst, send, recv, **device):
        return pltpu.make_async_remote_copy(
            src_ref=src, dst_ref=dst, send_sem=send, recv_sem=recv,
            device_id=device, device_id_type=MESH,
        )

    def token_copy(j, level):
        return remote(tok, zbuf.at[level], zs.at[j], zr.at[level], tp=flip(z, j) * CORES + c)

    def gain_copy(i, part):
        return remote(gain, gains.at[part], gs.at[i], gr.at[part], tp=flip(t, i))

    def row_copy(j, d, source):
        level = flip(z, j)
        return remote(
            xsend.at[j, d], x.at[level * CORES + c, source],
            xs.at[j, d], xr.at[level, source], ep=flip(e, d),
        )

    def core_copy(level, source, core):
        slot = x.at[level * CORES + core, source]
        return remote(slot, slot, fs.at[level, source], fr.at[level, source], tp=z * CORES + 1 - c)

    def half_copy(source):
        return remote(
            half.at[source], half_in.at[source], ds.at[source], dr.at[source],
            tp=z * CORES + 1 - c,
        )

    def back_copy(level, source, expert):
        return remote(
            back.at[source, level], ret.at[level, expert],
            qs.at[source, level], qr.at[level, expert], ep=source,
        )

    def sum_copy(j, level):
        return remote(zsend.at[j], zin.at[level], cs.at[j], cr.at[level], tp=flip(z, j) * CORES + c)

    def stat_copy(i, part):
        return remote(stats.at[t], stats.at[part], ps.at[i], pr.at[part], tp=flip(t, i))

    zbuf[z] = tok[...]
    gains[t] = gain[...]
    r = route[...]
    first, second = r[0:1], r[1:2]
    w = weight[...]
    names = lax.broadcasted_iota(jnp.int32, (8, rows), 0)
    member = jnp.where((names == first) | (names == second), 1.0, 0.0)
    before = jnp.where(
        lax.broadcasted_iota(jnp.int32, (rows, rows), 0)
        < lax.broadcasted_iota(jnp.int32, (rows, rows), 1),
        1.0, 0.0,
    )
    slots = jnp.dot(member.astype(BF16), before.astype(BF16), preferred_element_type=F32)
    slots = jnp.where(member > 0.5, slots, -1.0).astype(jnp.int32)
    lines = lax.broadcasted_iota(jnp.int32, (cap, rows), 0)
    for k in range(groups):
        disp[k] = jnp.where(lines == slots[k : k + 1], 1.0, 0.0).astype(BF16)

    pl.semaphore_wait(barrier, parts + groups - 2)
    for j in range(1, levels):
        token_copy(j, z).start()

    def send(j):
        level = flip(z, j)
        if j > 0:
            token_copy(j, level).wait_recv()
        block = zbuf[level]
        for d in range(groups - 1, -1, -1):
            picked = jnp.dot(disp[flip(e, d)], block, preferred_element_type=F32).astype(BF16)
            if d:
                xsend[j, d] = picked
                row_copy(j, d, e).start()
            else:
                x[level * CORES + c, e] = picked
                core_copy(level, e, c).start()

    def pass_on(j):
        level = flip(z, j)
        for d in range(groups - 1, 0, -1):
            source = flip(e, d)
            row_copy(j, d, source).wait_recv()
            core_copy(level, source, c).start()

    def project(j, source):
        level = flip(z, j)
        core_copy(level, source, 1 - c).wait_recv()
        total, gate_part, up_part = None, None, None
        for core in range(CORES):
            part = level * CORES + core
            values = x[part, source].astype(F32)
            square = values * values
            for lane in range(0, width, 128):
                piece = square[:, lane : lane + 128]
                total = piece if total is None else total + piece
            scaled = (values * gains[part]).astype(BF16)
            depth = pl.ds(pl.multiple_of(part * width, 128), width)
            gate_new = jnp.dot(scaled, gate[depth, :], preferred_element_type=F32)
            up_new = jnp.dot(scaled, up[depth, :], preferred_element_type=F32)
            gate_part = gate_new if gate_part is None else gate_part + gate_new
            up_part = up_new if up_part is None else up_part + up_new
        if j > 0:
            total = total + squares[source]
            gate_part = gate_part + acc_gate[source]
            up_part = up_part + acc_up[source]
        return total, gate_part, up_part

    def collect(j):
        def body(i, carry):
            source = flip_traced(e, groups - 1 - i, groups)
            squares[source], acc_gate[source], acc_up[source] = project(j, source)
            return carry

        pass_on(j)
        lax.fori_loop(0, groups, body, 0)

    send(0)
    for i in range(1, parts):
        gain_copy(i, t).start()
    for k in range(groups):
        chosen = jnp.where(first == k, w[0:1], w[1:2])
        mix[k * cap : (k + 1) * cap, :] = jnp.where(lines == slots[k : k + 1], chosen, 0.0)
    turned = mix[...].T
    high = turned.astype(BF16)
    hi[...] = high
    lo[...] = (turned - high.astype(F32)).astype(BF16)
    for j in range(1, levels):
        send(j)
        if j == 1:
            for i in range(1, parts):
                gain_copy(i, flip(t, i)).wait_recv()
            loads[0].wait()
            loads[1].wait()
        collect(j - 1)

    def reduce(source):
        half_copy(source).wait_recv()
        for j in range(levels - 1, -1, -1):
            level = flip(z, j)
            summed = (own[source, level] + half_in[source, level].astype(F32)).astype(BF16)
            yield j, level, summed

    def expert(i, carry):
        source = flip_traced(e, groups - 1 - i, groups)
        total, gate_part, up_part = project(levels - 1, source)
        scale = lax.rsqrt(jnp.sum(total, axis=1, keepdims=True) / full + EPSILON)
        gate_part = gate_part * scale
        hidden[...] = (
            gate_part / (1.0 + jnp.exp(-gate_part)) * (up_part * scale)
        ).astype(BF16)

        def down_block(level, core):
            columns = pl.ds(pl.multiple_of((level * CORES + core) * width, 128), width)
            return jnp.dot(hidden[...], down[:, columns], preferred_element_type=F32)

        for level in range(levels):
            half[source, level] = down_block(level, 1 - c).astype(BF16)
        half_copy(source).start()
        for level in range(levels):
            own[source, level] = down_block(level, c)

        @pl.when(i > 0)
        def _():
            earlier = flip_traced(e, groups - i, groups)
            for _, level, summed in reduce(earlier):
                back[earlier, level] = summed
                back_copy(level, earlier, e).start()

        return carry

    pass_on(levels - 1)
    loads[2].wait()
    lax.fori_loop(0, groups, expert, 0)
    for _, level, summed in reduce(e):
        ret[level, e] = summed

    combined = None
    for j in range(levels - 1, -1, -1):
        level = flip(z, j)
        for d in range(groups - 1, 0, -1):
            source = flip(e, d)
            back_copy(level, source, source).wait_recv()
        results = ret[level].reshape(groups * cap, width)
        combined = jnp.dot(hi[...], results, preferred_element_type=F32) + jnp.dot(
            lo[...], results, preferred_element_type=F32
        )
        if j:
            zsend[j] = combined.astype(BF16)
            sum_copy(j, z).start()
    for j in range(levels - 1, 0, -1):
        level = flip(z, j)
        sum_copy(j, level).wait_recv()
        combined = combined + zin[level].astype(F32)
    stats[t] = lax.dot_general(
        jnp.ones((8, width), F32), combined * combined, (((1,), (1,)), ((), ())),
        precision=EXACT, preferred_element_type=F32,
    )
    for i in range(1, parts):
        stat_copy(i, t).start()
    for i in range(1, parts):
        stat_copy(i, flip(t, i)).wait_recv()
    total = jnp.sum(stats[...], axis=0)
    column = lax.dot_general(
        total, jnp.full((8, 128), 0.125, F32), (((0,), (0,)), ((), ())),
        precision=EXACT, preferred_element_type=F32,
    )
    scale = lax.rsqrt(column[:, 0:1] / full + EPSILON)
    out[...] = (combined * scale * post[...]).astype(BF16)

    for j in range(1, levels):
        token_copy(j, z).wait_send()
        sum_copy(j, z).wait_send()
    for i in range(1, parts):
        gain_copy(i, t).wait_send()
        stat_copy(i, t).wait_send()
    for j in range(levels):
        for d in range(1, groups):
            row_copy(j, d, e).wait_send()
            back_copy(j, flip(e, d), e).wait_send()
        for k in range(groups):
            core_copy(j, k, c).wait_send()
    for k in range(groups):
        half_copy(k).wait_send()


def local_fused(tokens, pre_gain, expert_gate, expert_up, expert_down, routes, route_weights, post_gain):
    groups, parts = lax.axis_size("ep"), lax.axis_size("tp")
    rows, width = tokens.shape
    _, features, units = expert_gate.shape
    levels = parts // CORES
    cap = 3 * rows // groups
    vmem = pl.BlockSpec(memory_space=pltpu.VMEM)
    anywhere = pl.BlockSpec(memory_space=pl.ANY)
    dma = pltpu.SemaphoreType.DMA
    block = (levels, groups, cap, width)
    by_source = (groups, levels, cap, width)
    return pl.pallas_call(
        functools.partial(fused, groups, parts),
        out_shape=jax.ShapeDtypeStruct((rows, width), BF16),
        in_specs=[vmem] * 4 + [anywhere] * 3 + [vmem],
        out_specs=vmem,
        scratch_shapes=[
            pltpu.VMEM((levels, rows, width), BF16),
            pltpu.VMEM((parts, 1, width), F32),
            pltpu.VMEM((groups, cap, rows), BF16),
            pltpu.VMEM((groups * cap, rows), F32),
            pltpu.VMEM((rows, groups * cap), BF16),
            pltpu.VMEM((rows, groups * cap), BF16),
            pltpu.VMEM(block, BF16),
            pltpu.VMEM((parts, groups, cap, width), BF16),
            pltpu.VMEM((groups, cap, 128), F32),
            pltpu.VMEM((features, units), BF16),
            pltpu.VMEM((features, units), BF16),
            pltpu.VMEM((units, features), BF16),
            pltpu.VMEM((groups, cap, units), F32),
            pltpu.VMEM((groups, cap, units), F32),
            pltpu.VMEM((cap, units), BF16),
            pltpu.VMEM(by_source, BF16),
            pltpu.VMEM(by_source, F32),
            pltpu.VMEM(by_source, BF16),
            pltpu.VMEM(by_source, BF16),
            pltpu.VMEM(block, BF16),
            pltpu.VMEM((levels, rows, width), BF16),
            pltpu.VMEM((levels, rows, width), BF16),
            pltpu.VMEM((parts, 8, rows), F32),
            dma((3,)),
            dma((levels,)), dma((levels,)),
            dma((parts,)), dma((parts,)),
            dma((levels, groups)), dma((levels, groups)),
            dma((levels, groups)), dma((levels, groups)),
            dma((groups,)), dma((groups,)),
            dma((groups, levels)), dma((levels, groups)),
            dma((levels,)), dma((levels,)),
            dma((parts,)), dma((parts,)),
        ],
        compiler_params=pltpu.CompilerParams(
            collective_id=0, has_side_effects=True, vmem_limit_bytes=60 * 1024 * 1024
        ),
    )(
        tokens, pre_gain.reshape(1, width), routes.T, route_weights.T,
        expert_gate, expert_up, expert_down, post_gain.reshape(1, width),
    )


def power_of_two(count):
    return count & (count - 1) == 0


def plan(mesh):
    def choose(*args):
        tokens, gate = args[0], args[2]
        groups, parts = mesh.shape["ep"], mesh.shape["tp"]
        rows, width = tokens.shape
        fits = (
            gate.shape[0] == 1
            and power_of_two(groups)
            and power_of_two(parts)
            and 2 <= groups <= 8
            and parts >= 2 * CORES
            and width % 128 == 0
            and rows % 128 == 0
            and (3 * rows // groups) % 16 == 0
            and (3 * rows) % 128 == 0
            and gate.shape[2] % 128 == 0
        )
        return (local_fused if fits else local)(*args)

    return choose


def solution(mesh):
    placed = (
        P("ep", "tp"),
        P("tp"),
        P("ep", None, "tp"),
        P("ep", None, "tp"),
        P("ep", "tp", None),
        P("ep", None),
        P("ep", None),
        P("tp"),
    )
    return jax.shard_map(
        plan(mesh), mesh=mesh, in_specs=placed, out_specs=P("ep", "tp"), check_vma=False
    )
```

```python
import functools

import jax
import jax.numpy as jnp
from jax import lax
from jax.experimental import pallas as pl
from jax.experimental.pallas import tpu as pltpu
from jax.sharding import PartitionSpec as P

EPSILON = 1e-06


def local(tokens, pre_gain, expert_gate, expert_up, expert_down, routes, route_weights, post_gain):
    local_experts = expert_gate.shape[0]
    groups = lax.axis_size("ep")
    experts_all = local_experts * groups
    tok_rows, part_width = tokens.shape
    full_width = part_width * lax.axis_size("tp")
    capacity = 3 * tok_rows // experts_all
    values = tokens.astype(jnp.float32)
    input_sq = lax.psum(jnp.sum(values * values, axis=-1), "tp")
    normed = (
        values * lax.rsqrt(input_sq / full_width + EPSILON)[:, None] * pre_gain[None, :]
    ).astype(jnp.bfloat16)
    onehot = (routes[:, :, None] == jnp.arange(experts_all, dtype=jnp.int32)).astype(jnp.int32)
    onehot = onehot.reshape(tok_rows * 2, experts_all)
    earlier = jnp.cumsum(onehot, axis=0) - onehot
    slots = jnp.sum(earlier * onehot, axis=-1).reshape(tok_rows, 2)
    positions = routes * capacity + slots
    places = jnp.arange(experts_all * capacity, dtype=jnp.int32)
    first_pick = (places[:, None] == positions[None, :, 0]).astype(jnp.bfloat16)
    second_pick = (places[:, None] == positions[None, :, 1]).astype(jnp.bfloat16)
    dispatch = first_pick + second_pick
    outgoing = jnp.dot(dispatch, normed, preferred_element_type=jnp.float32).astype(jnp.bfloat16)
    arrived = lax.all_to_all(outgoing, "ep", split_axis=0, concat_axis=0, tiled=True)
    fragment = lax.all_gather(arrived, "tp", axis=1, tiled=True)
    count = fragment.shape[1]
    grouped = fragment.reshape(groups, local_experts, capacity, count)
    gate_pre = jnp.einsum(
        "secw,ewf->secf", grouped, expert_gate, preferred_element_type=jnp.float32
    )
    up_pre = jnp.einsum("secw,ewf->secf", grouped, expert_up, preferred_element_type=jnp.float32)
    hidden = (jax.nn.silu(gate_pre) * up_pre).astype(jnp.bfloat16)
    product = jnp.einsum("secf,efd->dsec", hidden, expert_down, preferred_element_type=jnp.float32)
    summed = lax.psum_scatter(
        product.reshape(lax.axis_size("tp") * part_width, groups * local_experts * capacity).astype(
            jnp.bfloat16
        ),
        "tp",
        scatter_dimension=0,
        tiled=True,
    )
    returned = lax.all_to_all(summed, "ep", split_axis=1, concat_axis=1, tiled=True)
    contract = (((0,), (1,)), ((), ()))
    first_out = lax.dot_general(first_pick, returned, contract, preferred_element_type=jnp.float32)
    second_out = lax.dot_general(
        second_pick, returned, contract, preferred_element_type=jnp.float32
    )
    combined = route_weights[:, 0:1] * first_out + route_weights[:, 1:2] * second_out
    output_sq = lax.psum(jnp.sum(combined * combined, axis=-1), "tp")
    scaled = combined * lax.rsqrt(output_sq / full_width + EPSILON)[:, None] * post_gain[None, :]
    return scaled.astype(jnp.bfloat16)


CORES = 2
F32 = jnp.float32
BF16 = jnp.bfloat16
EXACT = lax.Precision.HIGHEST
MESH = pl.DeviceIdType.MESH


def flip(index, bits):
    place = 1
    while place <= bits:
        if bits & place:
            index = index + place - 2 * place * lax.rem(lax.div(index, place), 2)
        place *= 2
    return index


def flip_traced(index, bits, size):
    total, place = 0, 1
    while place < size:
        total = total + place * lax.rem(lax.div(index, place) + lax.div(bits, place), 2)
        place *= 2
    return total


def fused(
    groups, parts, tok, gain, route, weight, gate_hbm, up_hbm, down_hbm, post, out,
    zbuf, gains, disp, mix, hi, lo, xsend, x, squares, gate, up, down, acc_gate, acc_up,
    hidden, half, own, half_in, back, ret, zsend, zin, stats,
    wsem, zs, zr, gs, gr, xs, xr, fs, fr, ds, dr, qs, qr, cs, cr, ps, pr,
):
    t, e = lax.axis_index("tp"), lax.axis_index("ep")
    z, c = lax.div(t, CORES), lax.rem(t, CORES)
    levels = parts // CORES
    rows, width = tok.shape
    cap = disp.shape[1]
    full = parts * width

    barrier = pltpu.get_barrier_semaphore()
    for i in range(1, parts):
        pl.semaphore_signal(barrier, inc=1, device_id={"tp": flip(t, i)}, device_id_type=MESH)
    for d in range(1, groups):
        pl.semaphore_signal(barrier, inc=1, device_id={"ep": flip(e, d)}, device_id_type=MESH)

    loads = [
        pltpu.make_async_copy(gate_hbm.at[0], gate, wsem.at[0]),
        pltpu.make_async_copy(up_hbm.at[0], up, wsem.at[1]),
        pltpu.make_async_copy(down_hbm.at[0], down, wsem.at[2]),
    ]
    for load in loads:
        load.start()

    def remote(src, dst, send, recv, **device):
        return pltpu.make_async_remote_copy(
            src_ref=src, dst_ref=dst, send_sem=send, recv_sem=recv,
            device_id=device, device_id_type=MESH,
        )

    def token_copy(level, up):
        step = 1 if up else -1
        source = zbuf.at[level]
        return remote(source, source, zs.at[level, int(up)], zr.at[level], tp=t + step * CORES)

    def relay(k):
        @pl.when(z >= k)
        def _():
            if k:
                token_copy(z - k, True).wait_recv()

            @pl.when(z < levels - 1)
            def _():
                token_copy(z - k, True).start()

        @pl.when(z + k < levels)
        def _():
            if k:
                token_copy(z + k, False).wait_recv()

            @pl.when(z > 0)
            def _():
                token_copy(z + k, False).start()

    def gain_copy(i, part):
        return remote(gain, gains.at[part], gs.at[i], gr.at[part], tp=flip(t, i))

    def row_copy(j, d, source):
        level = flip(z, j)
        return remote(
            xsend.at[j, d], x.at[level * CORES + c, source],
            xs.at[j, d], xr.at[level, source], ep=flip(e, d),
        )

    def core_copy(level, source, core):
        slot = x.at[level * CORES + core, source]
        return remote(slot, slot, fs.at[level, source], fr.at[level, source], tp=z * CORES + 1 - c)

    def half_copy(source):
        return remote(
            half.at[source], half_in.at[source], ds.at[source], dr.at[source],
            tp=z * CORES + 1 - c,
        )

    def back_copy(level, source, expert):
        return remote(
            back.at[source, level], ret.at[level, expert],
            qs.at[source, level], qr.at[level, expert], ep=source,
        )

    def sum_copy(j, level):
        return remote(zsend.at[j], zin.at[level], cs.at[j], cr.at[level], tp=flip(z, j) * CORES + c)

    def stat_copy(i, part):
        return remote(stats.at[t], stats.at[part], ps.at[i], pr.at[part], tp=flip(t, i))

    zbuf[z] = tok[...]
    gains[t] = gain[...]
    r = route[...]
    first, second = r[0:1], r[1:2]
    w = weight[...]
    names = lax.broadcasted_iota(jnp.int32, (8, rows), 0)
    member = jnp.where((names == first) | (names == second), 1.0, 0.0)
    before = jnp.where(
        lax.broadcasted_iota(jnp.int32, (rows, rows), 0)
        < lax.broadcasted_iota(jnp.int32, (rows, rows), 1),
        1.0, 0.0,
    )
    slots = jnp.dot(member.astype(BF16), before.astype(BF16), preferred_element_type=F32)
    slots = jnp.where(member > 0.5, slots, -1.0).astype(jnp.int32)
    lines = lax.broadcasted_iota(jnp.int32, (cap, rows), 0)
    for k in range(groups):
        disp[k] = jnp.where(lines == slots[k : k + 1], 1.0, 0.0).astype(BF16)

    pl.semaphore_wait(barrier, parts + groups - 2)
    relay(0)

    def send(j):
        level = flip(z, j)
        if j > 0:
            relay(j)
        block = zbuf[level]
        for d in range(groups - 1, -1, -1):
            picked = jnp.dot(disp[flip(e, d)], block, preferred_element_type=F32).astype(BF16)
            if d:
                xsend[j, d] = picked
                row_copy(j, d, e).start()
            else:
                x[level * CORES + c, e] = picked
                core_copy(level, e, c).start()

    def pass_on(j):
        level = flip(z, j)
        for d in range(groups - 1, 0, -1):
            source = flip(e, d)
            row_copy(j, d, source).wait_recv()
            core_copy(level, source, c).start()

    def project(j, source):
        level = flip(z, j)
        core_copy(level, source, 1 - c).wait_recv()
        total, gate_part, up_part = None, None, None
        for core in range(CORES):
            part = level * CORES + core
            values = x[part, source].astype(F32)
            square = values * values
            for lane in range(0, width, 128):
                piece = square[:, lane : lane + 128]
                total = piece if total is None else total + piece
            scaled = (values * gains[part]).astype(BF16)
            depth = pl.ds(pl.multiple_of(part * width, 128), width)
            gate_new = jnp.dot(scaled, gate[depth, :], preferred_element_type=F32)
            up_new = jnp.dot(scaled, up[depth, :], preferred_element_type=F32)
            gate_part = gate_new if gate_part is None else gate_part + gate_new
            up_part = up_new if up_part is None else up_part + up_new
        if j > 0:
            total = total + squares[source]
            gate_part = gate_part + acc_gate[source]
            up_part = up_part + acc_up[source]
        return total, gate_part, up_part

    def collect(j):
        def body(i, carry):
            source = flip_traced(e, groups - 1 - i, groups)
            squares[source], acc_gate[source], acc_up[source] = project(j, source)
            return carry

        pass_on(j)
        lax.fori_loop(0, groups, body, 0)

    send(0)
    for i in range(1, parts):
        gain_copy(i, t).start()
    for k in range(groups):
        chosen = jnp.where(first == k, w[0:1], w[1:2])
        mix[k * cap : (k + 1) * cap, :] = jnp.where(lines == slots[k : k + 1], chosen, 0.0)
    turned = mix[...].T
    high = turned.astype(BF16)
    hi[...] = high
    lo[...] = (turned - high.astype(F32)).astype(BF16)
    for j in range(1, levels):
        send(j)
        if j == 1:
            for i in range(1, parts):
                gain_copy(i, flip(t, i)).wait_recv()
            loads[0].wait()
            loads[1].wait()
        collect(j - 1)

    def reduce(source):
        half_copy(source).wait_recv()
        for j in range(levels - 1, -1, -1):
            level = flip(z, j)
            summed = (own[source, level] + half_in[source, level].astype(F32)).astype(BF16)
            yield j, level, summed

    def expert(i, carry):
        source = flip_traced(e, groups - 1 - i, groups)
        total, gate_part, up_part = project(levels - 1, source)
        scale = lax.rsqrt(jnp.sum(total, axis=1, keepdims=True) / full + EPSILON)
        gate_part = gate_part * scale
        hidden[...] = (
            gate_part / (1.0 + jnp.exp(-gate_part)) * (up_part * scale)
        ).astype(BF16)

        def down_block(level, core):
            columns = pl.ds(pl.multiple_of((level * CORES + core) * width, 128), width)
            return jnp.dot(hidden[...], down[:, columns], preferred_element_type=F32)

        for level in range(levels):
            half[source, level] = down_block(level, 1 - c).astype(BF16)
        half_copy(source).start()
        for level in range(levels):
            own[source, level] = down_block(level, c)

        @pl.when(i > 0)
        def _():
            earlier = flip_traced(e, groups - i, groups)
            for _, level, summed in reduce(earlier):
                back[earlier, level] = summed
                back_copy(level, earlier, e).start()

        return carry

    pass_on(levels - 1)
    loads[2].wait()
    lax.fori_loop(0, groups, expert, 0)
    for _, level, summed in reduce(e):
        ret[level, e] = summed

    combined = None
    for j in range(levels - 1, -1, -1):
        level = flip(z, j)
        for d in range(groups - 1, 0, -1):
            source = flip(e, d)
            back_copy(level, source, source).wait_recv()
        results = ret[level].reshape(groups * cap, width)
        combined = jnp.dot(hi[...], results, preferred_element_type=F32) + jnp.dot(
            lo[...], results, preferred_element_type=F32
        )
        if j:
            zsend[j] = combined.astype(BF16)
            sum_copy(j, z).start()
    for j in range(levels - 1, 0, -1):
        level = flip(z, j)
        sum_copy(j, level).wait_recv()
        combined = combined + zin[level].astype(F32)
    stats[t] = lax.dot_general(
        jnp.ones((8, width), F32), combined * combined, (((1,), (1,)), ((), ())),
        precision=EXACT, preferred_element_type=F32,
    )
    for i in range(1, parts):
        stat_copy(i, t).start()
    for i in range(1, parts):
        stat_copy(i, flip(t, i)).wait_recv()
    total = jnp.sum(stats[...], axis=0)
    column = lax.dot_general(
        total, jnp.full((8, 128), 0.125, F32), (((0,), (0,)), ((), ())),
        precision=EXACT, preferred_element_type=F32,
    )
    scale = lax.rsqrt(column[:, 0:1] / full + EPSILON)
    out[...] = (combined * scale * post[...]).astype(BF16)

    for j in range(levels):

        @pl.when((z >= j) & (z < levels - 1))
        def _():
            token_copy(j, True).wait_send()

        @pl.when((z <= j) & (z > 0))
        def _():
            token_copy(j, False).wait_send()

    for j in range(1, levels):
        sum_copy(j, z).wait_send()
    for i in range(1, parts):
        gain_copy(i, t).wait_send()
        stat_copy(i, t).wait_send()
    for j in range(levels):
        for d in range(1, groups):
            row_copy(j, d, e).wait_send()
            back_copy(j, flip(e, d), e).wait_send()
        for k in range(groups):
            core_copy(j, k, c).wait_send()
    for k in range(groups):
        half_copy(k).wait_send()


def local_fused(tokens, pre_gain, expert_gate, expert_up, expert_down, routes, route_weights, post_gain):
    groups, parts = lax.axis_size("ep"), lax.axis_size("tp")
    rows, width = tokens.shape
    _, features, units = expert_gate.shape
    levels = parts // CORES
    cap = 3 * rows // groups
    vmem = pl.BlockSpec(memory_space=pltpu.VMEM)
    anywhere = pl.BlockSpec(memory_space=pl.ANY)
    dma = pltpu.SemaphoreType.DMA
    block = (levels, groups, cap, width)
    by_source = (groups, levels, cap, width)
    return pl.pallas_call(
        functools.partial(fused, groups, parts),
        out_shape=jax.ShapeDtypeStruct((rows, width), BF16),
        in_specs=[vmem] * 4 + [anywhere] * 3 + [vmem],
        out_specs=vmem,
        scratch_shapes=[
            pltpu.VMEM((levels, rows, width), BF16),
            pltpu.VMEM((parts, 1, width), F32),
            pltpu.VMEM((groups, cap, rows), BF16),
            pltpu.VMEM((groups * cap, rows), F32),
            pltpu.VMEM((rows, groups * cap), BF16),
            pltpu.VMEM((rows, groups * cap), BF16),
            pltpu.VMEM(block, BF16),
            pltpu.VMEM((parts, groups, cap, width), BF16),
            pltpu.VMEM((groups, cap, 128), F32),
            pltpu.VMEM((features, units), BF16),
            pltpu.VMEM((features, units), BF16),
            pltpu.VMEM((units, features), BF16),
            pltpu.VMEM((groups, cap, units), F32),
            pltpu.VMEM((groups, cap, units), F32),
            pltpu.VMEM((cap, units), BF16),
            pltpu.VMEM(by_source, BF16),
            pltpu.VMEM(by_source, F32),
            pltpu.VMEM(by_source, BF16),
            pltpu.VMEM(by_source, BF16),
            pltpu.VMEM(block, BF16),
            pltpu.VMEM((levels, rows, width), BF16),
            pltpu.VMEM((levels, rows, width), BF16),
            pltpu.VMEM((parts, 8, rows), F32),
            dma((3,)),
            dma((levels, 2)), dma((levels,)),
            dma((parts,)), dma((parts,)),
            dma((levels, groups)), dma((levels, groups)),
            dma((levels, groups)), dma((levels, groups)),
            dma((groups,)), dma((groups,)),
            dma((groups, levels)), dma((levels, groups)),
            dma((levels,)), dma((levels,)),
            dma((parts,)), dma((parts,)),
        ],
        compiler_params=pltpu.CompilerParams(
            collective_id=0, has_side_effects=True, vmem_limit_bytes=60 * 1024 * 1024
        ),
    )(
        tokens, pre_gain.reshape(1, width), routes.T, route_weights.T,
        expert_gate, expert_up, expert_down, post_gain.reshape(1, width),
    )


def power_of_two(count):
    return count & (count - 1) == 0


def plan(mesh):
    def choose(*args):
        tokens, gate = args[0], args[2]
        groups, parts = mesh.shape["ep"], mesh.shape["tp"]
        rows, width = tokens.shape
        fits = (
            gate.shape[0] == 1
            and power_of_two(groups)
            and power_of_two(parts)
            and 2 <= groups <= 8
            and parts >= 2 * CORES
            and width % 128 == 0
            and rows % 128 == 0
            and (3 * rows // groups) % 16 == 0
            and (3 * rows) % 128 == 0
            and gate.shape[2] % 128 == 0
        )
        return (local_fused if fits else local)(*args)

    return choose


def solution(mesh):
    placed = (
        P("ep", "tp"),
        P("tp"),
        P("ep", None, "tp"),
        P("ep", None, "tp"),
        P("ep", "tp", None),
        P("ep", None),
        P("ep", None),
        P("tp"),
    )
    return jax.shard_map(
        plan(mesh), mesh=mesh, in_specs=placed, out_specs=P("ep", "tp"), check_vma=False
    )
```
